32 devices in a mesh: sp: 8 (over z, x), tp: 4 (over y, core).
Axes of the slice: x: 2, y: 2, z: 4, core: 2. Of those that a mesh axis runs over, the one named last changes fastest.
Arguments:
- query_matrix: bfloat16 [2048, 1024], P('sp', 'tp'), may hold values from -6 to 6
- key_matrix: bfloat16 [2048, 1024], P('sp', 'tp'), may hold values from -6 to 6
- value_matrix: bfloat16 [2048, 2048], P('sp', 'tp'), may hold values from -6 to 6
- output_gate_rows: bfloat16 [2048, 2048], P('sp', 'tp'), may hold values from -6 to 6
- decay_preactivation: bfloat16 [2048, 1024], P('sp', 'tp'), may hold values from -5 to 5
- channel_decay_bias: float32 [1024], P('tp'), may hold values from 0 to 10
- extra_log_decay: float32 [2048, 16], P('sp', 'tp'), may hold values from -0.7 to 0
- head_norm_gain: float32 [128], replicated, may hold values from 0.1 to 1.9
- output_projection: bfloat16 [2048, 2048], P('tp'), may hold values from -0.125 to 0.125
- residual_input: bfloat16 [2048, 2048], P(('sp', 'tp')), may hold values from -6 to 6
- attention_norm_gain: float32 [2048], replicated, may hold values from 0.1 to 1.9
- expert_before_gain: float32 [2048], replicated, may hold values from 0.1 to 1.9
- expert_after_gain: float32 [2048], replicated, may hold values from 0.1 to 1.9
- expert_gate_weight: bfloat16 [8, 2048, 4096], P('sp', None, 'tp'), may hold values from -0.125 to 0.125
- expert_up_weight: bfloat16 [8, 2048, 4096], P('sp', None, 'tp'), may hold values from -0.125 to 0.125
- expert_down_weight: bfloat16 [8, 4096, 2048], P('sp', 'tp'), may hold values from -0.09375 to 0.09375
- token_expert_index: int32 [2048, 2], P('sp'), may hold values from 0 to 7, as said below
- routing_weight_matrix: float32 [2048, 2], P('sp'), may hold values from 0.1 to 1
Outputs:
- layer_out: bfloat16 [2048, 2048], P(('sp', 'tp'))
The draws below stay inside these ranges and needn't reach their ends.
Inputs may be any that keep to these rules, and one draw needn't show every extreme that they name: `token_expert_index`: the 2 experts of a token differ and lie in one group: they have the same value of e // 4. In each aligned block of 256 rows (the rows of one index of sp) no expert is named by more than 80 rows, and the 4 experts of one group are each named by exactly 80 rows in every block.
All inputs are finite; a program needn't handle non-finite values.
Results may differ from the reference program's by a relative error of at most 0.024.
Values may be sent and summed in bfloat16 or wider, within the bound.
A program may use at most 64 MiB of HBM per device.

```python
import jax
import jax.numpy as jnp
from jax import lax

D = 2048
HEAD_TOTAL = 16
KEY_CHANNELS = 64
DV = 128
FF = 4096
GROUP_SIZE = 4
TOP = 2
BLOCK = 64
TOK_DEV = 256
SEQUENCE_TOKENS = 2048
KEYW = 1024
VALW = 2048
EXPERTS = 8
N_SP = 8
N_TP = 4


def draw_decay_preactivation(key, part):
    noise_key, shift_key = jax.random.split(jax.random.fold_in(key, 12))
    block_count = SEQUENCE_TOKENS // TOK_DEV
    noise = jnp.clip(jax.random.normal(noise_key, (block_count, TOK_DEV, KEYW), jnp.float32), -4.0, 4.0)
    shift = jax.random.uniform(shift_key, (block_count, 1, KEYW), jnp.float32, -1.0, 1.0)
    return (noise + shift).reshape(SEQUENCE_TOKENS, KEYW).astype(jnp.bfloat16)


def draw_channel_decay_bias(key, part):
    pick_key, fast_key, slow_key = jax.random.split(jax.random.fold_in(key, 11), 3)
    fast_share = 0.5
    fast_head = jax.random.uniform(pick_key, (HEAD_TOTAL, 1), jnp.float32) < fast_share
    fast_bias = jax.random.uniform(fast_key, (HEAD_TOTAL, KEY_CHANNELS), jnp.float32, 0.0, 1.0)
    slow_bias = jax.random.uniform(slow_key, (HEAD_TOTAL, KEY_CHANNELS), jnp.float32, 8.5, 10.0)
    return jnp.where(fast_head, fast_bias, slow_bias).reshape(HEAD_TOTAL * KEY_CHANNELS)


def draw_extra_log_decay(key, part):
    position_random_key, size_key = jax.random.split(jax.random.fold_in(key, 13))
    spike_positions = jax.random.randint(position_random_key, (3, HEAD_TOTAL), 0, SEQUENCE_TOKENS)
    kept_share = jax.random.uniform(size_key, (3, HEAD_TOTAL), jnp.float32, 0.5, 0.8)
    match_table = (jnp.arange(SEQUENCE_TOKENS)[:, None, None] == spike_positions[None]).astype(jnp.float32)
    return jnp.sum(match_table * jnp.log(kept_share)[None], axis=1)


def draw_token_expert_index(key, part):
    base_key = jax.random.fold_in(key, 14)
    group_count = N_SP // GROUP_SIZE
    capacity = 5 * TOK_DEV // (2 * N_SP)
    full_rows = 2 * capacity
    others = group_count - 1
    unit_count = (TOK_DEV - full_rows) // GROUP_SIZE
    full_group = jax.random.randint(jax.random.fold_in(base_key, 0), (), 0, group_count)
    mark_index = jnp.arange(others + 1, dtype=jnp.int32)
    marks_base = mark_index * unit_count // others
    interior = ((mark_index > 0) & (mark_index < others)).astype(jnp.int32)
    jitter = jax.random.randint(jax.random.fold_in(base_key, 1), (N_SP, others + 1), 0, 2) * interior[None, :]
    bounds = full_rows + GROUP_SIZE * (marks_base[None, :] + jitter)
    ranks = jnp.arange(TOK_DEV, dtype=jnp.int32)
    passed = jnp.sum((ranks[None, :, None] >= bounds[:, None, 1:others]).astype(jnp.int32), axis=2)
    group_start = jnp.take_along_axis(bounds, passed, axis=1)
    in_full = ranks[None, :] < full_rows
    local_rank = jnp.where(in_full, ranks[None, :], ranks[None, :] - group_start)
    group_id = jnp.where(in_full, full_group, passed + (passed >= full_group).astype(jnp.int32))
    offsets = jax.random.randint(jax.random.fold_in(base_key, 2), (N_SP, group_count), 0, GROUP_SIZE)
    strides = jax.random.randint(jax.random.fold_in(base_key, 3), (N_SP, group_count), 1, GROUP_SIZE)
    offset_row = jnp.take_along_axis(offsets, group_id, axis=1)
    stride_row = jnp.take_along_axis(strides, group_id, axis=1)
    first_expert = group_id * GROUP_SIZE + (local_rank + offset_row) % GROUP_SIZE
    second_expert = group_id * GROUP_SIZE + (local_rank + offset_row + stride_row) % GROUP_SIZE
    paired = jnp.stack([first_expert, second_expert], axis=-1)
    order_keys = jax.random.split(jax.random.fold_in(base_key, 4), N_SP)
    orders = jax.vmap(lambda order_key: jax.random.permutation(order_key, TOK_DEV))(order_keys)
    block_rows = jnp.arange(N_SP, dtype=jnp.int32)[:, None]
    placed = jnp.zeros_like(paired).at[block_rows, orders].set(paired)
    return placed.reshape(SEQUENCE_TOKENS, TOP).astype(jnp.int32)


def block_levels(rng, shape, shards, least, top_value):
    def one(axis_at, blocks):
        draws = jax.random.uniform(jax.random.fold_in(jax.random.fold_in(rng, 6), axis_at), (blocks,), jnp.float32, least / len(shards), top_value / len(shards))
        return jnp.repeat(jnp.exp(draws), shape[axis_at] // blocks).reshape((-1,) + (1,) * (len(shape) - axis_at - 1))

    loudness = one(*shards[0])
    for cut in shards[1:]:
        loudness = loudness * one(*cut)
    return loudness


def gaussian(key, extent, deviation, bound, cuts=(), kind=jnp.bfloat16):
    gain = block_levels(key, extent, cuts, -0.22, 0.18) if cuts else 1.0
    entries = jax.random.normal(key, extent, jnp.float32) * deviation * gain
    return jnp.minimum(jnp.maximum(entries, -bound), bound).astype(kind)


def setup_inputs(seed: int = 0) -> dict:
    streams_of = jax.random.split(jax.random.key(seed), 19)
    return {
        "query_matrix": gaussian(streams_of[0], (SEQUENCE_TOKENS, KEYW), 1.0, 6.0, ((0, 8), (1, 4))),
        "key_matrix": gaussian(streams_of[1], (SEQUENCE_TOKENS, KEYW), 1.0, 6.0, ((0, 8), (1, 4))),
        "value_matrix": gaussian(streams_of[2], (SEQUENCE_TOKENS, VALW), 1.0, 6.0, ((0, 8), (1, 4))),
        "output_gate_rows": gaussian(streams_of[3], (SEQUENCE_TOKENS, VALW), 1.0, 6.0, ((0, 8), (1, 4))),
        "decay_preactivation": draw_decay_preactivation(jax.random.fold_in(streams_of[18], 71), 0),
        "channel_decay_bias": draw_channel_decay_bias(jax.random.fold_in(streams_of[18], 71), 0),
        "extra_log_decay": draw_extra_log_decay(jax.random.fold_in(streams_of[18], 71), 0),
        "head_norm_gain": jnp.clip(1.0 + 0.18 * jax.random.normal(streams_of[7], (DV,), jnp.float32), 0.1, 1.9),
        "output_projection": gaussian(streams_of[8], (VALW, D), VALW ** -0.5, 0.125, ((0, 4),)),
        "residual_input": gaussian(streams_of[9], (SEQUENCE_TOKENS, D), 1.0, 6.0, ((0, 32),)),
        "attention_norm_gain": jnp.clip(1.0 + 0.18 * jax.random.normal(streams_of[10], (D,), jnp.float32), 0.1, 1.9),
        "expert_before_gain": jnp.clip(1.0 + 0.18 * jax.random.normal(streams_of[11], (D,), jnp.float32), 0.1, 1.9),
        "expert_after_gain": jnp.clip(1.0 + 0.18 * jax.random.normal(streams_of[12], (D,), jnp.float32), 0.1, 1.9),
        "expert_gate_weight": gaussian(streams_of[13], (EXPERTS, D, FF), D ** -0.5, 0.125, ((0, 8), (2, 4))),
        "expert_up_weight": gaussian(streams_of[14], (EXPERTS, D, FF), D ** -0.5, 0.125, ((0, 8), (2, 4))),
        "expert_down_weight": gaussian(streams_of[15], (EXPERTS, FF, D), FF ** -0.5, 0.09375, ((0, 8), (1, 4))),
        "token_expert_index": draw_token_expert_index(jax.random.fold_in(streams_of[18], 71), 0),
        "routing_weight_matrix": jnp.clip(0.1 + 0.9 * jax.random.uniform(streams_of[17], (SEQUENCE_TOKENS, TOP), jnp.float32) ** block_levels(streams_of[17], (SEQUENCE_TOKENS, TOP), ((0, 8),), -0.2, 0.2), 0.1, 1.0),
    }


EPSILON = 1e-06
DECAY_NORMALIZER = 16.0
HIGHEST = lax.Precision.HIGHEST

def rms_scale(values, gain_row):
    return values * lax.rsqrt(lax.optimization_barrier(jnp.mean(values * values, axis=-1, keepdims=True)) + EPSILON) * gain_row

def rounded(values):
    return lax.optimization_barrier(values.astype(jnp.bfloat16)).astype(jnp.float32)

def blockwise_state(queries, keys_all, values_all, decay_logarithm):
    sequence_length, number_heads, width_k = queries.shape
    width_v = values_all.shape[-1]
    blocks = sequence_length // BLOCK
    q_blocks = queries.reshape(blocks, BLOCK, number_heads, width_k)
    k_blocks = keys_all.reshape(blocks, BLOCK, number_heads, width_k)
    v_blocks = values_all.reshape(blocks, BLOCK, number_heads, width_v)
    inside = jnp.cumsum(decay_logarithm.reshape(blocks, BLOCK, number_heads, width_k), axis=1)
    block_end = inside[:, -1:]
    q_decayed = q_blocks * jnp.exp(inside)
    k_inverse = k_blocks * jnp.exp(-inside)
    k_to_end = k_blocks * jnp.exp(block_end - inside)
    causal = jnp.tril(jnp.ones((BLOCK, BLOCK), dtype=bool))
    scores = jnp.einsum('nihd,njhd->nhij', q_decayed, k_inverse, precision=HIGHEST)
    scores = jnp.where(causal, scores, 0.0)
    within = jnp.einsum('nhij,njhv->nihv', scores, v_blocks, precision=HIGHEST)
    growth = jnp.einsum('nchd,nchv->nhdv', k_to_end, v_blocks, precision=HIGHEST)
    fade_rows = jnp.exp(block_end[:, 0])

    def advance(running_state, inputs_pair):
        fade_now, grow_now = inputs_pair
        return (fade_now[..., None] * running_state + grow_now, running_state)
    zero_state = jnp.zeros((number_heads, width_k, width_v), jnp.float32)
    _, starts = lax.scan(advance, zero_state, (fade_rows, growth))
    across = jnp.einsum('nchd,nhdv->nchv', q_decayed, starts, precision=HIGHEST)
    return (within + across).reshape(sequence_length, number_heads, width_v)

def reference(query_matrix, key_matrix, value_matrix, output_gate_rows, decay_preactivation, channel_decay_bias, extra_log_decay, head_norm_gain, output_projection, residual_input, attention_norm_gain, expert_before_gain, expert_after_gain, expert_gate_weight, expert_up_weight, expert_down_weight, token_expert_index, routing_weight_matrix):
    sequence_length = query_matrix.shape[0]
    number_heads = value_matrix.shape[1] // DV
    model_width = residual_input.shape[1]
    queries = query_matrix.astype(jnp.float32).reshape(sequence_length, number_heads, KEY_CHANNELS) * KEY_CHANNELS ** (-0.5)
    keys_all = key_matrix.astype(jnp.float32).reshape(sequence_length, number_heads, KEY_CHANNELS)
    values_all = value_matrix.astype(jnp.float32).reshape(sequence_length, number_heads, DV)
    decay_logarithm = jax.nn.log_sigmoid(decay_preactivation.astype(jnp.float32) + channel_decay_bias) / DECAY_NORMALIZER
    decay_logarithm = decay_logarithm.reshape(sequence_length, number_heads, KEY_CHANNELS) + extra_log_decay[:, :, None]
    attn = blockwise_state(queries, keys_all, values_all, decay_logarithm)
    gate_act = jax.nn.silu(output_gate_rows.astype(jnp.float32).reshape(sequence_length, number_heads, DV))
    gated = (rms_scale(attn, head_norm_gain) * gate_act).astype(jnp.bfloat16)
    per_group = number_heads // N_TP
    grouped = gated.reshape(sequence_length, N_TP, per_group * DV).transpose(1, 0, 2)
    group_weights = output_projection.reshape(N_TP, per_group * DV, model_width)

    def add_group(total_sum, pair_in):
        group_rows, group_weight = pair_in
        return (total_sum + rounded(jnp.dot(group_rows, group_weight, preferred_element_type=jnp.float32)), None)
    mixed, _ = lax.scan(add_group, jnp.zeros((sequence_length, model_width), jnp.float32), (grouped, group_weights))
    layer_mid = (residual_input.astype(jnp.float32) + rms_scale(mixed, attention_norm_gain)).astype(jnp.bfloat16)
    normed = rms_scale(layer_mid.astype(jnp.float32), expert_before_gain).astype(jnp.bfloat16)
    expert_count = N_SP
    capacity = 5 * TOK_DEV // (2 * expert_count)
    block_ids = token_expert_index.reshape(N_SP, TOK_DEV * TOP)
    one_hot = (block_ids[:, :, None] == jnp.arange(expert_count, dtype=jnp.int32)[None, None, :]).astype(jnp.int32)
    slot_index = lax.optimization_barrier(jnp.sum((jnp.cumsum(one_hot, axis=1) - one_hot) * one_hot, axis=2))
    block_index = jnp.arange(N_SP, dtype=jnp.int32)[:, None]
    target = (block_ids * N_SP + block_index) * capacity + slot_index
    owners = jnp.zeros((expert_count * N_SP * capacity,), jnp.int32)
    owners = owners.at[target.reshape(-1)].set(jnp.arange(sequence_length * TOP, dtype=jnp.int32) // TOP)
    owners = owners.reshape(expert_count, N_SP * capacity)
    shard_width = FF // N_TP

    def run_expert(pack):
        row_index, w_gate, w_up, w_down = pack
        rows_in = normed[row_index]
        gate_part = jnp.dot(rows_in, w_gate, preferred_element_type=jnp.float32)
        up_part = jnp.dot(rows_in, w_up, preferred_element_type=jnp.float32)
        hidden = (jax.nn.silu(gate_part) * up_part).astype(jnp.bfloat16)
        hidden_parts = hidden.reshape(rows_in.shape[0], N_TP, shard_width).transpose(1, 0, 2)
        down_parts = w_down.reshape(N_TP, shard_width, model_width)

        def add_part(total_sum, pair_in):
            part_rows, part_weight = pair_in
            return (total_sum + rounded(jnp.dot(part_rows, part_weight, preferred_element_type=jnp.float32)), None)
        summed, _ = lax.scan(add_part, jnp.zeros((rows_in.shape[0], model_width), jnp.float32), (hidden_parts, down_parts))
        return summed.astype(jnp.bfloat16)
    served = lax.map(run_expert, (owners, expert_gate_weight, expert_up_weight, expert_down_weight))
    picked = served.reshape(-1, model_width)[target.reshape(sequence_length, TOP)].astype(jnp.float32)
    branch = lax.optimization_barrier(jnp.sum(routing_weight_matrix[:, :, None] * picked, axis=1))
    return (layer_mid.astype(jnp.float32) + rms_scale(branch, expert_after_gain)).astype(jnp.bfloat16)
```

```python
import functools

import jax
import jax.numpy as jnp
from jax import lax
from jax.experimental import pallas as pl
from jax.experimental.pallas import tpu as pltpu
from jax.sharding import PartitionSpec as P

KEY_CHANNELS = 64
DV = 128
TOP = 2
BLOCK = 64

EPSILON = 1e-06
DECAY_NORMALIZER = 16.0
HIGHEST = lax.Precision.HIGHEST
MESH = pl.DeviceIdType.MESH
F32 = jnp.float32
BF16 = jnp.bfloat16
FADE_ROWS = 16


def rms_scale(values, gain_row):
    return (
        values * lax.rsqrt(jnp.mean(values * values, axis=-1, keepdims=True) + EPSILON) * gain_row
    )


def contract(a, b, da, db):
    return lax.dot_general(a, b, (((da,), (db,)), ((), ())), preferred_element_type=F32)


def loop(count, body):
    def step(i, carry):
        body(i)
        return carry

    lax.fori_loop(0, count, step, 0)


def remote(src, dst, send, recv, device):
    return pltpu.make_async_remote_copy(
        src_ref=src,
        dst_ref=dst,
        send_sem=send,
        recv_sem=recv,
        device_id=device,
        device_id_type=MESH,
    )


def attention_kernel(
    n_sp, q_ref, k_ref, v_ref, g_ref, d_ref, bias_ref, extra_ref, hgain_ref, w_ref,
    out_ref, message, inbox, carried, gated, send_sem, recv_sem,
):
    me = lax.axis_index("sp")
    barrier = pltpu.get_barrier_semaphore()

    def greet(i):
        @pl.when(me - 1 - i >= 0)
        def _():
            pl.semaphore_signal(
                barrier, inc=1, device_id={"sp": jnp.maximum(me - 1 - i, 0)}, device_id_type=MESH
            )

    loop(n_sp - 1, greet)

    length, width = q_ref.shape
    heads = width // KEY_CHANNELS
    blocks = length // BLOCK
    x = d_ref[...].astype(F32) + bias_ref[...]
    log_decay = (jnp.minimum(x, 0.0) - jnp.log1p(jnp.exp(-jnp.abs(x)))) / DECAY_NORMALIZER
    extra = extra_ref[...]
    log_decay = log_decay + jnp.concatenate(
        [jnp.broadcast_to(extra[:, h : h + 1], (length, KEY_CHANNELS)) for h in range(heads)],
        axis=1,
    )
    row = lax.broadcasted_iota(jnp.int32, (length, length), 0)
    col = lax.broadcasted_iota(jnp.int32, (length, length), 1)
    causal = (row >= col) & (row // BLOCK == col // BLOCK)
    inside = jnp.dot(
        jnp.where(causal, 1.0, 0.0).astype(F32), log_decay, precision=HIGHEST,
        preferred_element_type=F32,
    )
    ends = [inside[(b + 1) * BLOCK - 1 : (b + 1) * BLOCK, :] for b in range(blocks)]
    offsets = [jnp.zeros_like(ends[0])]
    for b in range(blocks):
        offsets.append(offsets[-1] + ends[b])

    def spread(rows):
        return jnp.concatenate([jnp.broadcast_to(r, (BLOCK, width)) for r in rows], axis=0)

    q = q_ref[...].astype(F32) * KEY_CHANNELS ** (-0.5)
    k = k_ref[...].astype(F32)
    k_end = (k * jnp.exp(spread(ends) - inside)).astype(BF16)
    states = [jnp.zeros((DV, width), F32)]
    for b in range(blocks):
        rows = slice(b * BLOCK, (b + 1) * BLOCK)
        grown = jnp.concatenate(
            [
                contract(
                    v_ref[rows, h * DV : (h + 1) * DV],
                    k_end[rows, h * KEY_CHANNELS : (h + 1) * KEY_CHANNELS],
                    0,
                    0,
                )
                for h in range(heads)
            ],
            axis=1,
        )
        states.append(states[-1] * jnp.exp(ends[b]) + grown)
    message[0:DV, :] = states[-1].astype(BF16)
    message[DV:, :] = jnp.broadcast_to(jnp.exp(offsets[-1]), (FADE_ROWS, width)).astype(BF16)

    @pl.when(me < n_sp - 1)
    def _():
        pl.semaphore_wait(barrier, n_sp - 1 - me)

    def copy_of(i):
        return remote(
            message, inbox.at[me], send_sem.at[i], recv_sem.at[me],
            {"sp": jnp.minimum(me + 1 + i, n_sp - 1)},
        )

    def send(i):
        @pl.when(me + 1 + i < n_sp)
        def _():
            copy_of(i).start()

    loop(n_sp - 1, send)

    q_in = (q * jnp.exp(inside)).astype(BF16)
    k_inv = (k * jnp.exp(-inside)).astype(BF16)
    q_all = (q * jnp.exp(inside + spread(offsets[:-1]))).astype(BF16)
    local = []
    for h in range(heads):
        cs = slice(h * KEY_CHANNELS, (h + 1) * KEY_CHANNELS)
        scores = jnp.where(causal, contract(q_in[:, cs], k_inv[:, cs], 1, 1), 0.0).astype(BF16)
        within = jnp.dot(scores, v_ref[:, h * DV : (h + 1) * DV], preferred_element_type=F32)
        across = jnp.concatenate(
            [jnp.zeros((BLOCK, DV), F32)]
            + [
                contract(
                    q_in[b * BLOCK : (b + 1) * BLOCK, cs], states[b][:, cs].astype(BF16), 1, 1
                )
                for b in range(1, blocks)
            ],
            axis=0,
        )
        local.append(within + across)

    carried[...] = jnp.zeros_like(carried)

    def take(hop):
        @pl.when(hop < me)
        def _():
            remote(
                message, inbox.at[hop], send_sem.at[0], recv_sem.at[hop], {"sp": me}
            ).wait_recv()
            carried[...] = carried[...] * inbox[hop, DV : DV + 1, :].astype(F32) + inbox[
                hop, 0:DV, :
            ].astype(F32)

    loop(n_sp - 1, take)

    start = carried[...].astype(BF16)
    for h in range(heads):
        cs = slice(h * KEY_CHANNELS, (h + 1) * KEY_CHANNELS)
        vs = slice(h * DV, (h + 1) * DV)
        attn = local[h] + contract(q_all[:, cs], start[:, cs], 1, 1)
        gate = g_ref[:, vs].astype(F32)
        gated[:, vs] = (rms_scale(attn, hgain_ref[...]) * (gate * jax.nn.sigmoid(gate))).astype(
            BF16
        )
    out_ref[...] = jnp.dot(gated[...], w_ref[...], preferred_element_type=F32).astype(BF16)

    def drain(i):
        @pl.when(me + 1 + i < n_sp)
        def _():
            copy_of(i).wait_send()

    loop(n_sp - 1, drain)


def greet_all(n_sp, n_tp, me, j):
    barrier = pltpu.get_barrier_semaphore()

    def along_sp(i):
        pl.semaphore_signal(
            barrier, inc=1, device_id={"sp": lax.rem(me + 1 + i, n_sp)}, device_id_type=MESH
        )

    def along_tp(i):
        pl.semaphore_signal(
            barrier, inc=1, device_id={"tp": lax.rem(j + 1 + i, n_tp)}, device_id_type=MESH
        )

    loop(n_sp - 1, along_sp)
    loop(n_tp - 1, along_tp)
    pl.semaphore_wait(barrier, n_sp + n_tp - 2)


def dispatch_kernel(
    n_sp, n_tp, cap, part_ref, res_ref, again_ref, bgain_ref, target_ref,
    mid_ref, rows_ref,
    ra, rb, tb, normed, xcol, outgoing,
    sa, va, sb, vb, st, vt, ss, vs, sy, vy, sd, vd,
):
    me = lax.axis_index("sp")
    j = lax.axis_index("tp")
    n_y = n_tp // 2
    y, c = j // 2, lax.rem(j, 2)
    sibling = 2 * y + 1 - c
    rows = res_ref.shape[0]
    share = part_ref.shape[1] // n_tp
    greet_all(n_sp, n_tp, me, j)

    def rows_of(index):
        return pl.ds(pl.multiple_of(index * rows, rows), rows)

    def cols_of(index):
        return pl.ds(pl.multiple_of(index * share, share), share)

    def y_at(i):
        return lax.rem(y + 1 + i, n_y)

    def y_from(i):
        return lax.rem(y + n_y - 1 - i, n_y)

    def pair_copy(i):
        return remote(
            part_ref.at[rows_of(2 * y_at(i) + 1 - c)], ra.at[i], sa.at[i], va.at[i],
            {"tp": sibling},
        )

    def far_copy(i):
        return remote(tb.at[i], rb.at[i], sb.at[i], vb.at[i], {"tp": 2 * y_at(i) + c})

    loop(n_y, lambda i: pair_copy(i).start())

    def pair_sum(i):
        pair_copy(i).wait_recv()
        tb[i] = (
            part_ref[rows_of(2 * y_at(i) + c), :].astype(F32) + ra[i].astype(F32)
        ).astype(BF16)
        far_copy(i).start()

    loop(n_y - 1, pair_sum)
    pair_copy(n_y - 1).wait_recv()
    mixed = part_ref[rows_of(j), :].astype(F32) + ra[n_y - 1].astype(F32)
    for i in range(n_y - 1):
        far_copy(i).wait_recv()
        mixed = mixed + rb[i].astype(F32)
    mid = (res_ref[...].astype(F32) + rms_scale(mixed, again_ref[...])).astype(BF16)
    mid_ref[...] = mid
    normed[...] = rms_scale(mid.astype(F32), bgain_ref[...]).astype(BF16)

    def turn_copy(i):
        peer = lax.rem(j + 1 + i, n_tp)
        return remote(
            normed.at[:, cols_of(peer)], xcol.at[rows_of(j)], st.at[i], vt.at[i], {"tp": peer}
        )

    loop(n_tp - 1, lambda i: turn_copy(i).start())
    xcol[rows_of(j), :] = normed[:, cols_of(j)]
    loop(n_tp - 1, lambda i: turn_copy(i).wait_recv())

    x = xcol[...]
    t0, t1 = target_ref[0:1, :], target_ref[1:2, :]
    tokens = x.shape[0]

    def picked(expert):
        slot = lax.broadcasted_iota(jnp.int32, (cap, tokens), 0) + expert * cap
        chosen = jnp.where((slot == t0) | (slot == t1), 1.0, 0.0).astype(BF16)
        return jnp.dot(chosen, x, preferred_element_type=F32).astype(BF16)

    def out_copy(i):
        return remote(
            outgoing.at[i], rows_ref.at[me, :, cols_of(j)], ss.at[i], vs.at[i],
            {"sp": lax.rem(me + 1 + i, n_sp)},
        )

    def send(i):
        outgoing[i] = picked(lax.rem(me + 1 + i, n_sp))
        out_copy(i).start()

    loop(n_sp - 1, send)
    rows_ref[me, :, cols_of(j)] = picked(me)

    def source(i):
        return lax.rem(me + n_sp - i, n_sp)

    def y_copy(i, m):
        place = rows_ref.at[source(i), :, cols_of(j)]
        return remote(place, place, sy.at[m, i], vy.at[m, i], {"tp": 2 * y_at(m) + c})

    def pair_forward(i, m, owner):
        place = rows_ref.at[source(i), :, cols_of(owner)]
        return remote(place, place, sd.at[m, i], vd.at[m, i], {"tp": sibling})

    def arrived(i):
        @pl.when(i > 0)
        def _():
            out_copy(jnp.maximum(i - 1, 0)).wait_recv()

        for m in range(n_y - 1):
            y_copy(i, m).start()
        pair_forward(i, n_y - 1, j).start()

    loop(n_sp, arrived)

    def relay(i):
        for m in range(n_y - 1):
            y_copy(i, m).wait_recv()
            pair_forward(i, m, 2 * y_from(m) + c).start()

    loop(n_sp, relay)

    def finish(i):
        for m in range(n_y - 1):
            pair_forward(i, m, 2 * y_from(m) + c).wait()
            y_copy(i, m).wait_send()
        pair_forward(i, n_y - 1, j).wait()

    loop(n_sp, finish)

    def drain_pair(i):
        pair_copy(i).wait_send()

    loop(n_y, drain_pair)
    loop(n_y - 1, lambda i: far_copy(i).wait_send())
    loop(n_tp - 1, lambda i: turn_copy(i).wait_send())
    loop(n_sp - 1, lambda i: out_copy(i).wait_send())


def combine_kernel(
    n_sp, n_tp, cap, p_ref, mid_ref, gain_ref, target_ref, weight_ref,
    out_ref,
    r1, r2, tb, ob, back, turned, brow,
    s1, v1, s2, v2, s3, v3, s4, v4,
):
    me = lax.axis_index("sp")
    j = lax.axis_index("tp")
    n_y = n_tp // 2
    y, c = j // 2, lax.rem(j, 2)
    sibling = 2 * y + 1 - c
    rows = mid_ref.shape[0]
    share = p_ref.shape[2] // n_tp
    greet_all(n_sp, n_tp, me, j)

    def rows_of(index):
        return pl.ds(pl.multiple_of(index * rows, rows), rows)

    def cols_of(index):
        return pl.ds(pl.multiple_of(index * share, share), share)

    def y_at(i):
        return lax.rem(y + 1 + i, n_y)

    def block_of(i):
        return lax.rem(me + 1 + i, n_sp)

    def pair_copy(i, m):
        return remote(
            p_ref.at[block_of(i), :, cols_of(2 * y_at(m) + 1 - c)], r1.at[i, m],
            s1.at[i, m], v1.at[i, m], {"tp": sibling},
        )

    def far_copy(i, m):
        return remote(
            tb.at[i, m], r2.at[i, m], s2.at[i, m], v2.at[i, m], {"tp": 2 * y_at(m) + c}
        )

    def back_copy(i):
        return remote(ob.at[i], back.at[me], s3.at[i], v3.at[i], {"sp": block_of(i)})

    def first(i):
        for m in range(n_y):
            pair_copy(i, m).start()

    loop(n_sp, first)

    def second(i):
        for m in range(n_y - 1):
            pair_copy(i, m).wait_recv()
            tb[i, m] = (
                p_ref[block_of(i), :, cols_of(2 * y_at(m) + c)].astype(F32)
                + r1[i, m].astype(F32)
            ).astype(BF16)
            far_copy(i, m).start()

    loop(n_sp, second)

    def summed(i):
        pair_copy(i, n_y - 1).wait_recv()
        total = p_ref[block_of(i), :, cols_of(j)].astype(F32) + r1[i, n_y - 1].astype(F32)
        for m in range(n_y - 1):
            far_copy(i, m).wait_recv()
            total = total + r2[i, m].astype(F32)
        return total.astype(BF16)

    def third(i):
        ob[i] = summed(i)
        back_copy(i).start()

    loop(n_sp - 1, third)
    back[me] = summed(n_sp - 1)

    tokens = target_ref.shape[0]
    t0, t1 = target_ref[:, 0:1], target_ref[:, 1:2]
    w0, w1 = weight_ref[:, 0:1], weight_ref[:, 1:2]

    def weighed(expert):
        slot = lax.broadcasted_iota(jnp.int32, (tokens, cap), 1) + expert * cap
        mix = jnp.where(slot == t0, w0, 0.0) + jnp.where(slot == t1, w1, 0.0)
        high = mix.astype(BF16)
        low = (mix - high.astype(F32)).astype(BF16)
        served = back[expert]
        return jnp.dot(high, served, preferred_element_type=F32) + jnp.dot(
            low, served, preferred_element_type=F32
        )

    def gather(i, total):
        back_copy(i).wait_recv()
        return total + weighed(lax.rem(me + n_sp - 1 - i, n_sp))

    turned[...] = lax.fori_loop(0, n_sp - 1, gather, weighed(me)).astype(BF16)

    def turn_copy(i):
        peer = lax.rem(j + 1 + i, n_tp)
        return remote(
            turned.at[rows_of(peer)], brow.at[:, cols_of(j)], s4.at[i], v4.at[i], {"tp": peer}
        )

    loop(n_tp - 1, lambda i: turn_copy(i).start())
    brow[:, cols_of(j)] = turned[rows_of(j), :]
    loop(n_tp - 1, lambda i: turn_copy(i).wait_recv())
    out_ref[...] = (
        mid_ref[...].astype(F32) + rms_scale(brow[...].astype(F32), gain_ref[...])
    ).astype(BF16)

    def drain(i):
        for m in range(n_y):
            pair_copy(i, m).wait_send()
        for m in range(n_y - 1):
            far_copy(i, m).wait_send()

    loop(n_sp, drain)
    loop(n_sp - 1, lambda i: back_copy(i).wait_send())
    loop(n_tp - 1, lambda i: turn_copy(i).wait_send())


def call(kernel, operands, outs, scratch, ident, limit=48 << 20):
    vmem = pl.BlockSpec(memory_space=pltpu.VMEM)
    return pl.pallas_call(
        kernel,
        out_shape=outs,
        in_specs=[vmem] * len(operands),
        out_specs=jax.tree.map(lambda _: vmem, outs),
        scratch_shapes=scratch,
        compiler_params=pltpu.CompilerParams(
            collective_id=ident, has_side_effects=True, vmem_limit_bytes=limit
        ),
    )(*operands)


def dmas(*shapes):
    return [pltpu.SemaphoreType.DMA(s) for s in shapes]


def shards(
    n_sp,
    n_tp,
    query_matrix,
    key_matrix,
    value_matrix,
    output_gate_rows,
    decay_preactivation,
    channel_decay_bias,
    extra_log_decay,
    head_norm_gain,
    output_projection,
    residual_input,
    attention_norm_gain,
    expert_before_gain,
    expert_after_gain,
    expert_gate_weight,
    expert_up_weight,
    expert_down_weight,
    token_expert_index,
    routing_weight_matrix,
):
    length, width = query_matrix.shape
    model = output_projection.shape[1]
    rows = residual_input.shape[0]
    share = model // n_tp
    n_y = n_tp // 2
    capacity = 5 * length // (2 * n_sp)
    cap = (capacity + 15) // 16 * 16
    values = value_matrix.shape[1]

    flat = token_expert_index.reshape(length * TOP)
    one_hot = flat[:, None] == jnp.arange(n_sp, dtype=jnp.int32)[None, :]
    order = jnp.arange(length * TOP, dtype=jnp.int32)
    earlier = (order[:, None] > order[None, :]).astype(BF16)
    counts = jnp.dot(earlier, one_hot.astype(BF16), preferred_element_type=F32)
    slot = jnp.sum(jnp.where(one_hot, counts, 0.0), axis=1).astype(jnp.int32)
    target = (flat * cap + slot).reshape(length, TOP)

    part = call(
        functools.partial(attention_kernel, n_sp),
        (
            query_matrix,
            key_matrix,
            value_matrix,
            output_gate_rows,
            decay_preactivation,
            channel_decay_bias.reshape(1, width),
            extra_log_decay,
            head_norm_gain.reshape(1, DV),
            output_projection,
        ),
        jax.ShapeDtypeStruct((length, model), BF16),
        [
            pltpu.VMEM((DV + FADE_ROWS, width), BF16),
            pltpu.VMEM((n_sp, DV + FADE_ROWS, width), BF16),
            pltpu.VMEM((DV, width), F32),
            pltpu.VMEM((length, values), BF16),
        ]
        + dmas((n_sp,), (n_sp,)),
        1,
    )
    mid, rows_in = call(
        functools.partial(dispatch_kernel, n_sp, n_tp, cap),
        (
            part,
            residual_input,
            attention_norm_gain.reshape(1, model),
            expert_before_gain.reshape(1, model),
            target.T,
        ),
        (
            jax.ShapeDtypeStruct((rows, model), BF16),
            jax.ShapeDtypeStruct((n_sp, cap, model), BF16),
        ),
        [
            pltpu.VMEM((n_y, rows, model), BF16),
            pltpu.VMEM((n_y, rows, model), BF16),
            pltpu.VMEM((n_y, rows, model), BF16),
            pltpu.VMEM((rows, model), BF16),
            pltpu.VMEM((length, share), BF16),
            pltpu.VMEM((n_sp, cap, share), BF16),
        ]
        + dmas(
            (n_y,), (n_y,), (n_y,), (n_y,), (n_tp,), (n_tp,), (n_sp,), (n_sp,),
            (n_y, n_sp), (n_y, n_sp), (n_y, n_sp), (n_y, n_sp),
        ),
        2,
    )
    rows_in = rows_in.reshape(n_sp * cap, model)
    gate_part = jnp.dot(rows_in, expert_gate_weight[0], preferred_element_type=F32)
    up_part = jnp.dot(rows_in, expert_up_weight[0], preferred_element_type=F32)
    hidden = (jax.nn.silu(gate_part) * up_part).astype(BF16)
    partial_value = jnp.dot(hidden, expert_down_weight[0], preferred_element_type=F32)
    partial_value = partial_value.astype(BF16).reshape(n_sp, cap, model)
    return call(
        functools.partial(combine_kernel, n_sp, n_tp, cap),
        (
            partial_value,
            mid,
            expert_after_gain.reshape(1, model),
            target,
            routing_weight_matrix,
        ),
        jax.ShapeDtypeStruct((rows, model), BF16),
        [
            pltpu.VMEM((n_sp, n_y, cap, share), BF16),
            pltpu.VMEM((n_sp, n_y, cap, share), BF16),
            pltpu.VMEM((n_sp, n_y, cap, share), BF16),
            pltpu.VMEM((n_sp, cap, share), BF16),
            pltpu.VMEM((n_sp, cap, share), BF16),
            pltpu.VMEM((length, share), BF16),
            pltpu.VMEM((rows, model), BF16),
        ]
        + dmas(
            (n_sp, n_y), (n_sp, n_y), (n_sp, n_y), (n_sp, n_y), (n_sp,), (n_sp,), (n_tp,), (n_tp,)
        ),
        3,
    )


def solution(mesh):
    placed = (
        P("sp", "tp"),
        P("sp", "tp"),
        P("sp", "tp"),
        P("sp", "tp"),
        P("sp", "tp"),
        P("tp"),
        P("sp", "tp"),
        P(),
        P("tp", None),
        P(("sp", "tp"), None),
        P(),
        P(),
        P(),
        P("sp", None, "tp"),
        P("sp", None, "tp"),
        P("sp", "tp", None),
        P("sp", None),
        P("sp", None),
    )
    return jax.shard_map(
        functools.partial(shards, mesh.shape["sp"], mesh.shape["tp"]),
        mesh=mesh,
        in_specs=placed,
        out_specs=P(("sp", "tp"), None),
        check_vma=False,
    )
```

```python
import functools

import jax
import jax.numpy as jnp
from jax import lax
from jax.experimental import pallas as pl
from jax.experimental.pallas import tpu as pltpu
from jax.sharding import PartitionSpec as P

KEY_CHANNELS = 64
DV = 128
TOP = 2
BLOCK = 64

EPSILON = 1e-06
DECAY_NORMALIZER = 16.0
HIGHEST = lax.Precision.HIGHEST
MESH = pl.DeviceIdType.MESH
F32 = jnp.float32
BF16 = jnp.bfloat16
FADE_ROWS = 16


def rms_scale(values, gain_row):
    return (
        values * lax.rsqrt(jnp.mean(values * values, axis=-1, keepdims=True) + EPSILON) * gain_row
    )


def contract(a, b, da, db):
    return lax.dot_general(a, b, (((da,), (db,)), ((), ())), preferred_element_type=F32)


def loop(count, body):
    def step(i, carry):
        body(i)
        return carry

    lax.fori_loop(0, count, step, 0)


def remote(src, dst, send, recv, device):
    return pltpu.make_async_remote_copy(
        src_ref=src,
        dst_ref=dst,
        send_sem=send,
        recv_sem=recv,
        device_id=device,
        device_id_type=MESH,
    )


def attention_kernel(
    n_sp, q_hbm, k_hbm, v_hbm, g_hbm, d_hbm, bias_ref, extra_ref, hgain_ref, w_hbm,
    out_ref, message, inbox, carried, gated, q_ref, k_ref, v_ref, g_ref, d_ref, w_ref,
    send_sem, recv_sem, load_sem,
):
    me = lax.axis_index("sp")
    loads = [
        pltpu.make_async_copy(src, dst, load_sem.at[n])
        for n, (src, dst) in enumerate(
            (
                (d_hbm, d_ref),
                (k_hbm, k_ref),
                (v_hbm, v_ref),
                (q_hbm, q_ref),
                (g_hbm, g_ref),
                (w_hbm, w_ref),
            )
        )
    ]
    for copy in loads:
        copy.start()
    barrier = pltpu.get_barrier_semaphore()

    def greet(i):
        @pl.when(me - 1 - i >= 0)
        def _():
            pl.semaphore_signal(
                barrier, inc=1, device_id={"sp": jnp.maximum(me - 1 - i, 0)}, device_id_type=MESH
            )

    loop(n_sp - 1, greet)

    loads[0].wait()
    length, width = q_ref.shape
    heads = width // KEY_CHANNELS
    blocks = length // BLOCK
    x = d_ref[...].astype(F32) + bias_ref[...]
    log_decay = (jnp.minimum(x, 0.0) - jnp.log1p(jnp.exp(-jnp.abs(x)))) / DECAY_NORMALIZER
    extra = extra_ref[...]
    log_decay = log_decay + jnp.concatenate(
        [jnp.broadcast_to(extra[:, h : h + 1], (length, KEY_CHANNELS)) for h in range(heads)],
        axis=1,
    )
    row = lax.broadcasted_iota(jnp.int32, (length, length), 0)
    col = lax.broadcasted_iota(jnp.int32, (length, length), 1)
    causal = (row >= col) & (row // BLOCK == col // BLOCK)
    inside = jnp.dot(
        jnp.where(causal, 1.0, 0.0).astype(F32), log_decay, precision=HIGHEST,
        preferred_element_type=F32,
    )
    ends = [inside[(b + 1) * BLOCK - 1 : (b + 1) * BLOCK, :] for b in range(blocks)]
    offsets = [jnp.zeros_like(ends[0])]
    for b in range(blocks):
        offsets.append(offsets[-1] + ends[b])

    def spread(rows):
        return jnp.concatenate([jnp.broadcast_to(r, (BLOCK, width)) for r in rows], axis=0)

    for copy in loads[1:4]:
        copy.wait()
    q = q_ref[...].astype(F32) * KEY_CHANNELS ** (-0.5)
    k = k_ref[...].astype(F32)
    k_end = (k * jnp.exp(spread(ends) - inside)).astype(BF16)
    states = [jnp.zeros((DV, width), F32)]
    for b in range(blocks):
        rows = slice(b * BLOCK, (b + 1) * BLOCK)
        grown = jnp.concatenate(
            [
                contract(
                    v_ref[rows, h * DV : (h + 1) * DV],
                    k_end[rows, h * KEY_CHANNELS : (h + 1) * KEY_CHANNELS],
                    0,
                    0,
                )
                for h in range(heads)
            ],
            axis=1,
        )
        states.append(states[-1] * jnp.exp(ends[b]) + grown)
    message[0:DV, :] = states[-1].astype(BF16)
    message[DV:, :] = jnp.broadcast_to(jnp.exp(offsets[-1]), (FADE_ROWS, width)).astype(BF16)

    @pl.when(me < n_sp - 1)
    def _():
        pl.semaphore_wait(barrier, n_sp - 1 - me)

    def copy_of(i):
        return remote(
            message, inbox.at[me], send_sem.at[i], recv_sem.at[me],
            {"sp": jnp.minimum(me + 1 + i, n_sp - 1)},
        )

    def send(i):
        @pl.when(me + 1 + i < n_sp)
        def _():
            copy_of(i).start()

    loop(n_sp - 1, send)

    q_in = (q * jnp.exp(inside)).astype(BF16)
    k_inv = (k * jnp.exp(-inside)).astype(BF16)
    q_all = (q * jnp.exp(inside + spread(offsets[:-1]))).astype(BF16)
    local = []
    for h in range(heads):
        cs = slice(h * KEY_CHANNELS, (h + 1) * KEY_CHANNELS)
        scores = jnp.where(causal, contract(q_in[:, cs], k_inv[:, cs], 1, 1), 0.0).astype(BF16)
        within = jnp.dot(scores, v_ref[:, h * DV : (h + 1) * DV], preferred_element_type=F32)
        across = jnp.concatenate(
            [jnp.zeros((BLOCK, DV), F32)]
            + [
                contract(
                    q_in[b * BLOCK : (b + 1) * BLOCK, cs], states[b][:, cs].astype(BF16), 1, 1
                )
                for b in range(1, blocks)
            ],
            axis=0,
        )
        local.append(within + across)

    carried[...] = jnp.zeros_like(carried)

    def take(hop):
        @pl.when(hop < me)
        def _():
            remote(
                message, inbox.at[hop], send_sem.at[0], recv_sem.at[hop], {"sp": me}
            ).wait_recv()
            carried[...] = carried[...] * inbox[hop, DV : DV + 1, :].astype(F32) + inbox[
                hop, 0:DV, :
            ].astype(F32)

    loop(n_sp - 1, take)

    for copy in loads[4:]:
        copy.wait()
    start = carried[...].astype(BF16)
    for h in range(heads):
        cs = slice(h * KEY_CHANNELS, (h + 1) * KEY_CHANNELS)
        vs = slice(h * DV, (h + 1) * DV)
        attn = local[h] + contract(q_all[:, cs], start[:, cs], 1, 1)
        gate = g_ref[:, vs].astype(F32)
        gated[:, vs] = (rms_scale(attn, hgain_ref[...]) * (gate * jax.nn.sigmoid(gate))).astype(
            BF16
        )
    out_ref[...] = jnp.dot(gated[...], w_ref[...], preferred_element_type=F32).astype(BF16)

    def drain(i):
        @pl.when(me + 1 + i < n_sp)
        def _():
            copy_of(i).wait_send()

    loop(n_sp - 1, drain)


def greet_all(n_sp, n_tp, me, j):
    barrier = pltpu.get_barrier_semaphore()

    def along_sp(i):
        pl.semaphore_signal(
            barrier, inc=1, device_id={"sp": lax.rem(me + 1 + i, n_sp)}, device_id_type=MESH
        )

    def along_tp(i):
        pl.semaphore_signal(
            barrier, inc=1, device_id={"tp": lax.rem(j + 1 + i, n_tp)}, device_id_type=MESH
        )

    loop(n_sp - 1, along_sp)
    loop(n_tp - 1, along_tp)
    pl.semaphore_wait(barrier, n_sp + n_tp - 2)


def flipped(me, i, n):
    total, bit = 0, 1
    while bit < n:
        total = total + lax.rem(me // bit + i // bit, 2) * bit
        bit *= 2
    return total


def expert_kernel(
    n_sp, n_tp, cap, part_ref, res_hbm, again_ref, bgain_ref, fgain_ref, target_ref, turned_ref,
    weight_ref, wg_hbm, wu_hbm, wd_hbm,
    out_ref,
    res_ref, wg, wu, wd, ra, rb, tb, normed, xcol, outgoing, rows_ref, hidden, p_ref,
    r1, r2, ty, ob, back, branch, brow, mid_ref,
    load, sa, va, sb, vb, st, vt, ss, vs, sy, vy, sd, vd, s1, v1, s2, v2, s3, v3, s4, v4,
):
    me = lax.axis_index("sp")
    j = lax.axis_index("tp")
    n_y = n_tp // 2
    y, c = j // 2, lax.rem(j, 2)
    sibling = 2 * y + 1 - c
    rows, model = res_ref.shape
    share = model // n_tp
    half = n_sp // 2
    loads = [
        pltpu.make_async_copy(src, dst, load.at[n])
        for n, (src, dst) in enumerate(
            ((res_hbm, res_ref), (wg_hbm, wg), (wu_hbm, wu), (wd_hbm, wd))
        )
    ]
    for copy in loads:
        copy.start()
    greet_all(n_sp, n_tp, me, j)

    def rows_of(index):
        return pl.ds(pl.multiple_of(index * rows, rows), rows)

    def cols_of(index):
        return pl.ds(pl.multiple_of(index * share, share), share)

    def y_at(i):
        return lax.rem(y + 1 + i, n_y)

    def y_from(i):
        return lax.rem(y + n_y - 1 - i, n_y)

    def peer_of(i):
        return flipped(me, i, n_sp)

    def head_pair(i):
        return remote(
            part_ref.at[rows_of(2 * y_at(i) + 1 - c)], ra.at[i], sa.at[i], va.at[i],
            {"tp": sibling},
        )

    def head_far(i):
        return remote(tb.at[i], rb.at[i], sb.at[i], vb.at[i], {"tp": 2 * y_at(i) + c})

    loop(n_y, lambda i: head_pair(i).start())

    def pair_sum(i):
        head_pair(i).wait_recv()
        tb[i] = (
            part_ref[rows_of(2 * y_at(i) + c), :].astype(F32) + ra[i].astype(F32)
        ).astype(BF16)
        head_far(i).start()

    loop(n_y - 1, pair_sum)
    head_pair(n_y - 1).wait_recv()
    mixed = part_ref[rows_of(j), :].astype(F32) + ra[n_y - 1].astype(F32)
    loads[0].wait()
    for i in range(n_y - 1):
        head_far(i).wait_recv()
        mixed = mixed + rb[i].astype(F32)
    mid = (res_ref[...].astype(F32) + rms_scale(mixed, again_ref[...])).astype(BF16)
    mid_ref[...] = mid
    normed[...] = rms_scale(mid.astype(F32), bgain_ref[...]).astype(BF16)

    def turn_copy(i):
        peer = lax.rem(j + 1 + i, n_tp)
        return remote(
            normed.at[:, cols_of(peer)], xcol.at[rows_of(j)], st.at[i], vt.at[i], {"tp": peer}
        )

    loop(n_tp - 1, lambda i: turn_copy(i).start())
    xcol[rows_of(j), :] = normed[:, cols_of(j)]
    loop(n_tp - 1, lambda i: turn_copy(i).wait_recv())

    x = xcol[...]
    t0, t1 = turned_ref[0:1, :], turned_ref[1:2, :]
    tokens = x.shape[0]

    def picked(expert):
        slot = lax.broadcasted_iota(jnp.int32, (cap, tokens), 0) + expert * cap
        chosen = jnp.where((slot == t0) | (slot == t1), 1.0, 0.0).astype(BF16)
        return jnp.dot(chosen, x, preferred_element_type=F32).astype(BF16)

    def out_copy(i):
        return remote(
            outgoing.at[i], rows_ref.at[me, :, cols_of(j)], ss.at[i], vs.at[i],
            {"sp": peer_of(i)},
        )

    def send(i):
        outgoing[i + 1] = picked(peer_of(i + 1))
        out_copy(i + 1).start()

    loop(n_sp - 1, send)
    rows_ref[me, :, cols_of(j)] = picked(me)

    def y_copy(i, m):
        place = rows_ref.at[peer_of(i), :, cols_of(j)]
        return remote(place, place, sy.at[m, i], vy.at[m, i], {"tp": 2 * y_at(m) + c})

    def pair_forward(i, m, owner):
        place = rows_ref.at[peer_of(i), :, cols_of(owner)]
        return remote(place, place, sd.at[m, i], vd.at[m, i], {"tp": sibling})

    def forward(i):
        for m in range(n_y - 1):
            y_copy(i, m).start()
        pair_forward(i, n_y - 1, j).start()

    def arrived(i):
        out_copy(i).wait_recv()
        forward(i)

    def relay(i):
        for m in range(n_y - 1):
            y_copy(i, m).wait_recv()
            pair_forward(i, m, 2 * y_from(m) + c).start()

    def ready(i):
        for m in range(n_y - 1):
            pair_forward(i, m, 2 * y_from(m) + c).wait_recv()
        pair_forward(i, n_y - 1, j).wait_recv()

    def part_pair(i, m):
        return remote(
            p_ref.at[peer_of(i), :, cols_of(2 * y_at(m) + 1 - c)], r1.at[i, m],
            s1.at[i, m], v1.at[i, m], {"tp": sibling},
        )

    def part_far(i, m):
        return remote(
            ty.at[i, m], r2.at[i, m], s2.at[i, m], v2.at[i, m], {"tp": 2 * y_at(m) + c}
        )

    def back_copy(i):
        return remote(ob.at[i], back.at[me], s3.at[i], v3.at[i], {"sp": peer_of(i)})

    def pass_along(i, m):
        part_pair(i, m).wait_recv()
        ty[i, m] = (
            p_ref[peer_of(i), :, cols_of(2 * y_at(m) + c)].astype(F32) + r1[i, m].astype(F32)
        ).astype(BF16)
        part_far(i, m).start()

    def summed(i):
        part_pair(i, n_y - 1).wait_recv()
        total = p_ref[peer_of(i), :, cols_of(j)].astype(F32) + r1[i, n_y - 1].astype(F32)
        for m in range(n_y - 1):
            part_far(i, m).wait_recv()
            total = total + r2[i, m].astype(F32)
        return total.astype(BF16)

    def give_back(i):
        ob[i] = summed(i)
        back_copy(i).start()

    tile = min(256, wg.shape[1])
    steps = wg.shape[1] // tile

    def run_expert(first, during_up, during_down):
        blocks = pl.ds(peer_of(first) // half * half, half)
        batch = half * cap

        def up(t):
            cols = pl.ds(pl.multiple_of(t * tile, tile), tile)
            fed = rows_ref[blocks].reshape(batch, model)
            gate = jnp.dot(fed, wg[:, cols], preferred_element_type=F32)
            rise = jnp.dot(fed, wu[:, cols], preferred_element_type=F32)
            hidden[:, cols] = (gate * jax.nn.sigmoid(gate) * rise).astype(BF16)
            during_up(t)

        loop(steps, up)

        def down(owner):
            made = jnp.dot(hidden[...], wd[:, cols_of(owner)], preferred_element_type=F32)
            p_ref[blocks, :, cols_of(owner)] = made.astype(BF16).reshape(half, cap, share)

        def down_pair(m):
            down(2 * y_at(m) + 1 - c)
            loop(half, lambda i: part_pair(first + i, m).start())
            during_down(m)
            down(2 * y_at(m) + c)

            @pl.when(m < n_y - 1)
            def _():
                loop(half, lambda i: pass_along(first + i, m))

        loop(n_y, down_pair)

    def spaced(count, parts, body):
        each = -(-count // parts)

        def hook(t):
            def one(i):
                @pl.when(t * each + i < count)
                def _():
                    body(jnp.minimum(t * each + i, count - 1))

            loop(each, one)

        return hook

    forward(0)
    loop(half - 1, lambda i: arrived(i + 1))
    loop(half, relay)
    loop(half, ready)
    for copy in loads[1:]:
        copy.wait()
    run_expert(
        0,
        spaced(half, steps, lambda i: arrived(half + i)),
        spaced(half, n_y, lambda i: relay(half + i)),
    )
    loop(half, lambda i: ready(half + i))
    run_expert(
        half,
        spaced(half - 1, steps, lambda i: give_back(i + 1)),
        lambda m: None,
    )
    loop(half, lambda i: give_back(half + i))
    back[me] = summed(0)

    u0, u1 = target_ref[:, 0:1], target_ref[:, 1:2]
    w0, w1 = weight_ref[:, 0:1], weight_ref[:, 1:2]

    def weighed(expert):
        slot = lax.broadcasted_iota(jnp.int32, (tokens, cap), 1) + expert * cap
        mix = jnp.where(slot == u0, w0, 0.0) + jnp.where(slot == u1, w1, 0.0)
        high = mix.astype(BF16)
        low = (mix - high.astype(F32)).astype(BF16)
        served = back[expert]
        return jnp.dot(high, served, preferred_element_type=F32) + jnp.dot(
            low, served, preferred_element_type=F32
        )

    def gather(i, total):
        back_copy(i).wait_recv()
        return total + weighed(peer_of(i))

    branch[...] = lax.fori_loop(1, n_sp, gather, weighed(me)).astype(BF16)

    def home_copy(i):
        peer = lax.rem(j + 1 + i, n_tp)
        return remote(
            branch.at[rows_of(peer)], brow.at[:, cols_of(j)], s4.at[i], v4.at[i], {"tp": peer}
        )

    loop(n_tp - 1, lambda i: home_copy(i).start())
    brow[:, cols_of(j)] = branch[rows_of(j), :]
    loop(n_tp - 1, lambda i: home_copy(i).wait_recv())
    out_ref[...] = (
        mid_ref[...].astype(F32) + rms_scale(brow[...].astype(F32), fgain_ref[...])
    ).astype(BF16)

    loop(n_y, lambda i: head_pair(i).wait_send())
    loop(n_y - 1, lambda i: head_far(i).wait_send())
    loop(n_sp - 1, lambda i: out_copy(i + 1).wait_send())
    loop(n_sp - 1, lambda i: back_copy(i + 1).wait_send())

    def drain_turns(i):
        turn_copy(i).wait_send()
        home_copy(i).wait_send()

    loop(n_tp - 1, drain_turns)

    def drain(i):
        for m in range(n_y - 1):
            y_copy(i, m).wait_send()
            pair_forward(i, m, 2 * y_from(m) + c).wait_send()
            part_far(i, m).wait_send()
        pair_forward(i, n_y - 1, j).wait_send()
        for m in range(n_y):
            part_pair(i, m).wait_send()

    loop(n_sp, drain)


def call(kernel, operands, far, outs, scratch, ident, limit):
    vmem = pl.BlockSpec(memory_space=pltpu.VMEM)
    return pl.pallas_call(
        kernel,
        out_shape=outs,
        in_specs=[
            pl.BlockSpec(memory_space=pl.ANY) if n in far else vmem for n in range(len(operands))
        ],
        out_specs=jax.tree.map(lambda _: vmem, outs),
        scratch_shapes=scratch,
        compiler_params=pltpu.CompilerParams(
            collective_id=ident, has_side_effects=True, vmem_limit_bytes=limit
        ),
    )(*operands)


def dmas(*shapes):
    return [pltpu.SemaphoreType.DMA(s) for s in shapes]


def shards(
    n_sp,
    n_tp,
    query_matrix,
    key_matrix,
    value_matrix,
    output_gate_rows,
    decay_preactivation,
    channel_decay_bias,
    extra_log_decay,
    head_norm_gain,
    output_projection,
    residual_input,
    attention_norm_gain,
    expert_before_gain,
    expert_after_gain,
    expert_gate_weight,
    expert_up_weight,
    expert_down_weight,
    token_expert_index,
    routing_weight_matrix,
):
    length, width = query_matrix.shape
    model = output_projection.shape[1]
    rows = residual_input.shape[0]
    share = model // n_tp
    n_y = n_tp // 2
    capacity = 5 * length // (2 * n_sp)
    cap = (capacity + 15) // 16 * 16
    values = value_matrix.shape[1]

    flat = token_expert_index.reshape(length * TOP)
    one_hot = flat[:, None] == jnp.arange(n_sp, dtype=jnp.int32)[None, :]
    order = jnp.arange(length * TOP, dtype=jnp.int32)
    earlier = (order[:, None] > order[None, :]).astype(BF16)
    counts = jnp.dot(earlier, one_hot.astype(BF16), preferred_element_type=F32)
    slot = jnp.sum(jnp.where(one_hot, counts, 0.0), axis=1).astype(jnp.int32)
    target = (flat * cap + slot).reshape(length, TOP)

    part = call(
        functools.partial(attention_kernel, n_sp),
        (
            query_matrix,
            key_matrix,
            value_matrix,
            output_gate_rows,
            decay_preactivation,
            channel_decay_bias.reshape(1, width),
            extra_log_decay,
            head_norm_gain.reshape(1, DV),
            output_projection,
        ),
        (0, 1, 2, 3, 4, 8),
        jax.ShapeDtypeStruct((length, model), BF16),
        [
            pltpu.VMEM((DV + FADE_ROWS, width), BF16),
            pltpu.VMEM((n_sp, DV + FADE_ROWS, width), BF16),
            pltpu.VMEM((DV, width), F32),
            pltpu.VMEM((length, values), BF16),
            pltpu.VMEM((length, width), BF16),
            pltpu.VMEM((length, width), BF16),
            pltpu.VMEM((length, values), BF16),
            pltpu.VMEM((length, values), BF16),
            pltpu.VMEM((length, width), BF16),
            pltpu.VMEM((values, model), BF16),
        ]
        + dmas((n_sp,), (n_sp,), (6,)),
        1,
        32 << 20,
    )
    hidden_units = expert_gate_weight.shape[2]
    by_peer = (n_sp, n_y)
    return call(
        functools.partial(expert_kernel, n_sp, n_tp, cap),
        (
            part,
            residual_input,
            attention_norm_gain.reshape(1, model),
            expert_before_gain.reshape(1, model),
            expert_after_gain.reshape(1, model),
            target,
            target.T,
            routing_weight_matrix,
            expert_gate_weight[0],
            expert_up_weight[0],
            expert_down_weight[0],
        ),
        (1, 8, 9, 10),
        jax.ShapeDtypeStruct((rows, model), BF16),
        [
            pltpu.VMEM((rows, model), BF16),
            pltpu.VMEM((model, hidden_units), BF16),
            pltpu.VMEM((model, hidden_units), BF16),
            pltpu.VMEM((hidden_units, model), BF16),
            pltpu.VMEM((n_y, rows, model), BF16),
            pltpu.VMEM((n_y, rows, model), BF16),
            pltpu.VMEM((n_y, rows, model), BF16),
            pltpu.VMEM((rows, model), BF16),
            pltpu.VMEM((length, share), BF16),
            pltpu.VMEM((n_sp, cap, share), BF16),
            pltpu.VMEM((n_sp, cap, model), BF16),
            pltpu.VMEM((n_sp // 2 * cap, hidden_units), BF16),
            pltpu.VMEM((n_sp, cap, model), BF16),
            pltpu.VMEM(by_peer + (cap, share), BF16),
            pltpu.VMEM(by_peer + (cap, share), BF16),
            pltpu.VMEM(by_peer + (cap, share), BF16),
            pltpu.VMEM((n_sp, cap, share), BF16),
            pltpu.VMEM((n_sp, cap, share), BF16),
            pltpu.VMEM((length, share), BF16),
            pltpu.VMEM((rows, model), BF16),
            pltpu.VMEM((rows, model), BF16),
        ]
        + dmas(
            (4,), (n_y,), (n_y,), (n_y,), (n_y,), (n_tp,), (n_tp,), (n_sp,), (n_sp,),
            (n_y, n_sp), (n_y, n_sp), (n_y, n_sp), (n_y, n_sp),
            by_peer, by_peer, by_peer, by_peer, (n_sp,), (n_sp,), (n_tp,), (n_tp,),
        ),
        2,
        56 << 20,
    )


def solution(mesh):
    placed = (
        P("sp", "tp"),
        P("sp", "tp"),
        P("sp", "tp"),
        P("sp", "tp"),
        P("sp", "tp"),
        P("tp"),
        P("sp", "tp"),
        P(),
        P("tp", None),
        P(("sp", "tp"), None),
        P(),
        P(),
        P(),
        P("sp", None, "tp"),
        P("sp", None, "tp"),
        P("sp", "tp", None),
        P("sp", None),
        P("sp", None),
    )
    return jax.shard_map(
        functools.partial(shards, mesh.shape["sp"], mesh.shape["tp"]),
        mesh=mesh,
        in_specs=placed,
        out_specs=P(("sp", "tp"), None),
        check_vma=False,
    )
```

```python
import functools

import jax
import jax.numpy as jnp
from jax import lax
from jax.experimental import pallas as pl
from jax.experimental.pallas import tpu as pltpu
from jax.sharding import PartitionSpec as P

KEY_CHANNELS = 64
DV = 128
TOP = 2
BLOCK = 64

EPSILON = 1e-06
DECAY_NORMALIZER = 16.0
HIGHEST = lax.Precision.HIGHEST
MESH = pl.DeviceIdType.MESH
F32 = jnp.float32
BF16 = jnp.bfloat16
FADE_ROWS = 16


def rms_scale(values, gain_row):
    return (
        values * lax.rsqrt(jnp.mean(values * values, axis=-1, keepdims=True) + EPSILON) * gain_row
    )


def contract(a, b, da, db):
    return lax.dot_general(a, b, (((da,), (db,)), ((), ())), preferred_element_type=F32)


def loop(count, body):
    def step(i, carry):
        body(i)
        return carry

    lax.fori_loop(0, count, step, 0)


def remote(src, dst, send, recv, device):
    return pltpu.make_async_remote_copy(
        src_ref=src,
        dst_ref=dst,
        send_sem=send,
        recv_sem=recv,
        device_id=device,
        device_id_type=MESH,
    )


def attention_kernel(
    n_sp, q_hbm, k_hbm, v_hbm, g_hbm, d_hbm, bias_ref, extra_ref, hgain_ref, w_hbm,
    out_ref, message, inbox, carried, gated, q_ref, k_ref, v_ref, g_ref, d_ref, w_ref,
    send_sem, recv_sem, load_sem,
):
    me = lax.axis_index("sp")
    loads = [
        pltpu.make_async_copy(src, dst, load_sem.at[n])
        for n, (src, dst) in enumerate(
            (
                (d_hbm, d_ref),
                (k_hbm, k_ref),
                (v_hbm, v_ref),
                (q_hbm, q_ref),
                (g_hbm, g_ref),
                (w_hbm, w_ref),
            )
        )
    ]
    for copy in loads:
        copy.start()
    barrier = pltpu.get_barrier_semaphore()

    def greet(i):
        @pl.when(me - 1 - i >= 0)
        def _():
            pl.semaphore_signal(
                barrier, inc=1, device_id={"sp": jnp.maximum(me - 1 - i, 0)}, device_id_type=MESH
            )

    loop(n_sp - 1, greet)

    loads[0].wait()
    length, width = q_ref.shape
    heads = width // KEY_CHANNELS
    blocks = length // BLOCK
    x = d_ref[...].astype(F32) + bias_ref[...]
    log_decay = (jnp.minimum(x, 0.0) - jnp.log1p(jnp.exp(-jnp.abs(x)))) / DECAY_NORMALIZER
    extra = extra_ref[...]
    log_decay = log_decay + jnp.concatenate(
        [jnp.broadcast_to(extra[:, h : h + 1], (length, KEY_CHANNELS)) for h in range(heads)],
        axis=1,
    )
    row = lax.broadcasted_iota(jnp.int32, (length, length), 0)
    col = lax.broadcasted_iota(jnp.int32, (length, length), 1)
    causal = (row >= col) & (row // BLOCK == col // BLOCK)
    inside = jnp.dot(
        jnp.where(causal, 1.0, 0.0).astype(F32), log_decay, precision=HIGHEST,
        preferred_element_type=F32,
    )
    ends = [inside[(b + 1) * BLOCK - 1 : (b + 1) * BLOCK, :] for b in range(blocks)]
    offsets = [jnp.zeros_like(ends[0])]
    for b in range(blocks):
        offsets.append(offsets[-1] + ends[b])

    def spread(rows):
        return jnp.concatenate([jnp.broadcast_to(r, (BLOCK, width)) for r in rows], axis=0)

    for copy in loads[1:4]:
        copy.wait()
    q = q_ref[...].astype(F32) * KEY_CHANNELS ** (-0.5)
    k = k_ref[...].astype(F32)
    k_end = (k * jnp.exp(spread(ends) - inside)).astype(BF16)
    states = [jnp.zeros((DV, width), F32)]
    for b in range(blocks):
        rows = slice(b * BLOCK, (b + 1) * BLOCK)
        grown = jnp.concatenate(
            [
                contract(
                    v_ref[rows, h * DV : (h + 1) * DV],
                    k_end[rows, h * KEY_CHANNELS : (h + 1) * KEY_CHANNELS],
                    0,
                    0,
                )
                for h in range(heads)
            ],
            axis=1,
        )
        states.append(states[-1] * jnp.exp(ends[b]) + grown)
    message[0:DV, :] = states[-1].astype(BF16)
    message[DV:, :] = jnp.broadcast_to(jnp.exp(offsets[-1]), (FADE_ROWS, width)).astype(BF16)

    @pl.when(me < n_sp - 1)
    def _():
        pl.semaphore_wait(barrier, n_sp - 1 - me)

    def copy_of(i):
        return remote(
            message, inbox.at[me], send_sem.at[i], recv_sem.at[me],
            {"sp": jnp.minimum(me + 1 + i, n_sp - 1)},
        )

    def send(i):
        @pl.when(me + 1 + i < n_sp)
        def _():
            copy_of(i).start()

    loop(n_sp - 1, send)

    q_in = (q * jnp.exp(inside)).astype(BF16)
    k_inv = (k * jnp.exp(-inside)).astype(BF16)
    q_all = (q * jnp.exp(inside + spread(offsets[:-1]))).astype(BF16)
    local = []
    for h in range(heads):
        cs = slice(h * KEY_CHANNELS, (h + 1) * KEY_CHANNELS)
        scores = jnp.where(causal, contract(q_in[:, cs], k_inv[:, cs], 1, 1), 0.0).astype(BF16)
        within = jnp.dot(scores, v_ref[:, h * DV : (h + 1) * DV], preferred_element_type=F32)
        across = jnp.concatenate(
            [jnp.zeros((BLOCK, DV), F32)]
            + [
                contract(
                    q_in[b * BLOCK : (b + 1) * BLOCK, cs], states[b][:, cs].astype(BF16), 1, 1
                )
                for b in range(1, blocks)
            ],
            axis=0,
        )
        local.append(within + across)

    carried[...] = jnp.zeros_like(carried)

    def take(hop):
        @pl.when(hop < me)
        def _():
            remote(
                message, inbox.at[hop], send_sem.at[0], recv_sem.at[hop], {"sp": me}
            ).wait_recv()
            carried[...] = carried[...] * inbox[hop, DV : DV + 1, :].astype(F32) + inbox[
                hop, 0:DV, :
            ].astype(F32)

    loop(n_sp - 1, take)

    for copy in loads[4:]:
        copy.wait()
    start = carried[...].astype(BF16)
    for h in range(heads):
        cs = slice(h * KEY_CHANNELS, (h + 1) * KEY_CHANNELS)
        vs = slice(h * DV, (h + 1) * DV)
        attn = local[h] + contract(q_all[:, cs], start[:, cs], 1, 1)
        gate = g_ref[:, vs].astype(F32)
        gated[:, vs] = (rms_scale(attn, hgain_ref[...]) * (gate * jax.nn.sigmoid(gate))).astype(
            BF16
        )
    out_ref[...] = jnp.dot(gated[...], w_ref[...], preferred_element_type=F32).astype(BF16)

    def drain(i):
        @pl.when(me + 1 + i < n_sp)
        def _():
            copy_of(i).wait_send()

    loop(n_sp - 1, drain)


def greet_all(n_sp, n_tp, me, j):
    barrier = pltpu.get_barrier_semaphore()

    def along_sp(i):
        pl.semaphore_signal(
            barrier, inc=1, device_id={"sp": lax.rem(me + 1 + i, n_sp)}, device_id_type=MESH
        )

    def along_tp(i):
        pl.semaphore_signal(
            barrier, inc=1, device_id={"tp": lax.rem(j + 1 + i, n_tp)}, device_id_type=MESH
        )

    loop(n_sp - 1, along_sp)
    loop(n_tp - 1, along_tp)
    pl.semaphore_wait(barrier, n_sp + n_tp - 2)


def flipped(me, i, n):
    total, bit = 0, 1
    while bit < n:
        total = total + lax.rem(me // bit + i // bit, 2) * bit
        bit *= 2
    return total


def expert_kernel(
    n_sp, n_tp, cap, part_ref, res_hbm, again_ref, bgain_ref, fgain_ref, target_ref, turned_ref,
    weight_ref, wg_hbm, wu_hbm, wd_hbm,
    out_ref,
    res_ref, wg, wu, wd, ra, rb, tb, normed, xcol, outgoing, rows_ref, hidden, p_ref,
    r1, r2, ty, ob, back, branch, brow, mid_ref,
    load, sa, va, sb, vb, st, vt, ss, vs, sy, vy, sd, vd, s1, v1, s2, v2, s3, v3, s4, v4,
):
    me = lax.axis_index("sp")
    j = lax.axis_index("tp")
    n_y = n_tp // 2
    y, c = j // 2, lax.rem(j, 2)
    sibling = 2 * y + 1 - c
    rows, model = res_ref.shape
    share = model // n_tp
    half = n_sp // 2
    loads = [
        pltpu.make_async_copy(src, dst, load.at[n])
        for n, (src, dst) in enumerate(
            ((res_hbm, res_ref), (wg_hbm, wg), (wu_hbm, wu), (wd_hbm, wd))
        )
    ]
    for copy in loads:
        copy.start()
    greet_all(n_sp, n_tp, me, j)

    def rows_of(index):
        return pl.ds(pl.multiple_of(index * rows, rows), rows)

    def cols_of(index):
        return pl.ds(pl.multiple_of(index * share, share), share)

    def y_at(i):
        return lax.rem(y + 1 + i, n_y)

    def y_from(i):
        return lax.rem(y + n_y - 1 - i, n_y)

    def peer_of(i):
        return flipped(me, i, n_sp)

    def head_pair(i):
        return remote(
            part_ref.at[rows_of(2 * y_at(i) + 1 - c)], ra.at[i], sa.at[i], va.at[i],
            {"tp": sibling},
        )

    def head_far(i):
        return remote(tb.at[i], rb.at[i], sb.at[i], vb.at[i], {"tp": 2 * y_at(i) + c})

    loop(n_y, lambda i: head_pair(i).start())

    def pair_sum(i):
        head_pair(i).wait_recv()
        tb[i] = (
            part_ref[rows_of(2 * y_at(i) + c), :].astype(F32) + ra[i].astype(F32)
        ).astype(BF16)
        head_far(i).start()

    loop(n_y - 1, pair_sum)
    head_pair(n_y - 1).wait_recv()
    mixed = part_ref[rows_of(j), :].astype(F32) + ra[n_y - 1].astype(F32)
    loads[0].wait()
    for i in range(n_y - 1):
        head_far(i).wait_recv()
        mixed = mixed + rb[i].astype(F32)
    mid = (res_ref[...].astype(F32) + rms_scale(mixed, again_ref[...])).astype(BF16)
    mid_ref[...] = mid
    normed[...] = rms_scale(mid.astype(F32), bgain_ref[...]).astype(BF16)

    def turn_copy(i):
        peer = lax.rem(j + 1 + i, n_tp)
        return remote(
            normed.at[:, cols_of(peer)], xcol.at[rows_of(j)], st.at[i], vt.at[i], {"tp": peer}
        )

    loop(n_tp - 1, lambda i: turn_copy(i).start())
    xcol[rows_of(j), :] = normed[:, cols_of(j)]
    loop(n_tp - 1, lambda i: turn_copy(i).wait_recv())

    x = xcol[...]
    t0, t1 = turned_ref[0:1, :], turned_ref[1:2, :]
    tokens = x.shape[0]

    def picked(expert):
        slot = lax.broadcasted_iota(jnp.int32, (cap, tokens), 0) + expert * cap
        chosen = jnp.where((slot == t0) | (slot == t1), 1.0, 0.0).astype(BF16)
        return jnp.dot(chosen, x, preferred_element_type=F32).astype(BF16)

    def out_copy(i):
        return remote(
            outgoing.at[i], rows_ref.at[me, :, cols_of(j)], ss.at[i], vs.at[i],
            {"sp": peer_of(i)},
        )

    def send(i):
        outgoing[i + 1] = picked(peer_of(i + 1))
        out_copy(i + 1).start()

    loop(n_sp - 1, send)
    rows_ref[me, :, cols_of(j)] = picked(me)

    def y_copy(i, m):
        place = rows_ref.at[peer_of(i), :, cols_of(j)]
        return remote(place, place, sy.at[m, i], vy.at[m, i], {"tp": 2 * y_at(m) + c})

    def pair_forward(i, m, owner):
        place = rows_ref.at[peer_of(i), :, cols_of(owner)]
        return remote(place, place, sd.at[m, i], vd.at[m, i], {"tp": sibling})

    def forward(i):
        for m in range(n_y - 1):
            y_copy(i, m).start()
        pair_forward(i, n_y - 1, j).start()

    def arrived(i):
        out_copy(i).wait_recv()
        forward(i)

    def relay(i):
        for m in range(n_y - 1):
            y_copy(i, m).wait_recv()
            pair_forward(i, m, 2 * y_from(m) + c).start()

    def ready(i):
        for m in range(n_y - 1):
            pair_forward(i, m, 2 * y_from(m) + c).wait_recv()
        pair_forward(i, n_y - 1, j).wait_recv()

    def part_pair(i, m):
        return remote(
            p_ref.at[peer_of(i), :, cols_of(2 * y_at(m) + 1 - c)], r1.at[i, m],
            s1.at[i, m], v1.at[i, m], {"tp": sibling},
        )

    def part_far(i, m):
        return remote(
            ty.at[i, m], r2.at[i, m], s2.at[i, m], v2.at[i, m], {"tp": 2 * y_at(m) + c}
        )

    def back_copy(i):
        return remote(ob.at[i], back.at[me], s3.at[i], v3.at[i], {"sp": peer_of(i)})

    def pass_along(i, m):
        part_pair(i, m).wait_recv()
        ty[i, m] = (
            p_ref[peer_of(i), :, cols_of(2 * y_at(m) + c)].astype(F32) + r1[i, m].astype(F32)
        ).astype(BF16)
        part_far(i, m).start()

    def summed(i):
        part_pair(i, n_y - 1).wait_recv()
        total = p_ref[peer_of(i), :, cols_of(j)].astype(F32) + r1[i, n_y - 1].astype(F32)
        for m in range(n_y - 1):
            part_far(i, m).wait_recv()
            total = total + r2[i, m].astype(F32)
        return total.astype(BF16)

    def give_back(i):
        ob[i] = summed(i)
        back_copy(i).start()

    tile = min(256, wg.shape[1])
    steps = wg.shape[1] // tile

    def run_expert(first, during_up, during_down):
        blocks = pl.ds(peer_of(first) // half * half, half)
        batch = half * cap

        def up(t):
            cols = pl.ds(pl.multiple_of(t * tile, tile), tile)
            fed = rows_ref[blocks].reshape(batch, model)
            gate = jnp.dot(fed, wg[:, cols], preferred_element_type=F32)
            rise = jnp.dot(fed, wu[:, cols], preferred_element_type=F32)
            hidden[:, cols] = (gate * jax.nn.sigmoid(gate) * rise).astype(BF16)
            during_up(t)

        loop(steps, up)

        def down(owner):
            made = jnp.dot(hidden[...], wd[:, cols_of(owner)], preferred_element_type=F32)
            p_ref[blocks, :, cols_of(owner)] = made.astype(BF16).reshape(half, cap, share)

        def down_pair(m):
            down(2 * y_at(m) + 1 - c)
            loop(half, lambda i: part_pair(first + i, m).start())
            during_down(m)
            down(2 * y_at(m) + c)

            @pl.when(m < n_y - 1)
            def _():
                loop(half, lambda i: pass_along(first + i, m))

        loop(n_y, down_pair)

    def spaced(count, parts, body):
        each = -(-count // parts)

        def hook(t):
            def one(i):
                @pl.when(t * each + i < count)
                def _():
                    body(jnp.minimum(t * each + i, count - 1))

            loop(each, one)

        return hook

    forward(0)
    loop(half - 1, lambda i: arrived(i + 1))
    loop(half, relay)
    loop(half, ready)
    for copy in loads[1:]:
        copy.wait()
    run_expert(
        0,
        spaced(half, steps, lambda i: arrived(half + i)),
        spaced(half, n_y, lambda i: relay(half + i)),
    )
    loop(half, lambda i: ready(half + i))
    run_expert(
        half,
        spaced(half - 1, steps, lambda i: give_back(i + 1)),
        lambda m: None,
    )
    loop(half, lambda i: give_back(half + i))
    back[me] = summed(0)

    u0, u1 = target_ref[:, 0:1], target_ref[:, 1:2]
    w0, w1 = weight_ref[:, 0:1], weight_ref[:, 1:2]

    def weighed(expert):
        slot = lax.broadcasted_iota(jnp.int32, (tokens, cap), 1) + expert * cap
        mix = jnp.where(slot == u0, w0, 0.0) + jnp.where(slot == u1, w1, 0.0)
        high = mix.astype(BF16)
        low = (mix - high.astype(F32)).astype(BF16)
        served = back[expert]
        return jnp.dot(high, served, preferred_element_type=F32) + jnp.dot(
            low, served, preferred_element_type=F32
        )

    def gather(i, total):
        back_copy(i).wait_recv()
        return total + weighed(peer_of(i))

    branch[...] = lax.fori_loop(1, n_sp, gather, weighed(me)).astype(BF16)

    def home_copy(i):
        peer = lax.rem(j + 1 + i, n_tp)
        return remote(
            branch.at[rows_of(peer)], brow.at[:, cols_of(j)], s4.at[i], v4.at[i], {"tp": peer}
        )

    loop(n_tp - 1, lambda i: home_copy(i).start())
    brow[:, cols_of(j)] = branch[rows_of(j), :]
    loop(n_tp - 1, lambda i: home_copy(i).wait_recv())
    out_ref[...] = (
        mid_ref[...].astype(F32) + rms_scale(brow[...].astype(F32), fgain_ref[...])
    ).astype(BF16)

    loop(n_y, lambda i: head_pair(i).wait_send())
    loop(n_y - 1, lambda i: head_far(i).wait_send())
    loop(n_sp - 1, lambda i: out_copy(i + 1).wait_send())
    loop(n_sp - 1, lambda i: back_copy(i + 1).wait_send())

    def drain_turns(i):
        turn_copy(i).wait_send()
        home_copy(i).wait_send()

    loop(n_tp - 1, drain_turns)

    def drain(i):
        for m in range(n_y - 1):
            y_copy(i, m).wait_send()
            pair_forward(i, m, 2 * y_from(m) + c).wait_send()
            part_far(i, m).wait_send()
        pair_forward(i, n_y - 1, j).wait_send()
        for m in range(n_y):
            part_pair(i, m).wait_send()

    loop(n_sp, drain)


def call(kernel, operands, far, outs, scratch, ident, limit):
    vmem = pl.BlockSpec(memory_space=pltpu.VMEM)
    return pl.pallas_call(
        kernel,
        out_shape=outs,
        in_specs=[
            pl.BlockSpec(memory_space=pl.ANY) if n in far else vmem for n in range(len(operands))
        ],
        out_specs=jax.tree.map(lambda _: vmem, outs),
        scratch_shapes=scratch,
        compiler_params=pltpu.CompilerParams(
            collective_id=ident, has_side_effects=True, vmem_limit_bytes=limit
        ),
    )(*operands)


def dmas(*shapes):
    return [pltpu.SemaphoreType.DMA(s) for s in shapes]


def shards(
    n_sp,
    n_tp,
    query_matrix,
    key_matrix,
    value_matrix,
    output_gate_rows,
    decay_preactivation,
    channel_decay_bias,
    extra_log_decay,
    head_norm_gain,
    output_projection,
    residual_input,
    attention_norm_gain,
    expert_before_gain,
    expert_after_gain,
    expert_gate_weight,
    expert_up_weight,
    expert_down_weight,
    token_expert_index,
    routing_weight_matrix,
):
    length, width = query_matrix.shape
    model = output_projection.shape[1]
    rows = residual_input.shape[0]
    share = model // n_tp
    n_y = n_tp // 2
    capacity = 5 * length // (2 * n_sp)
    cap = (capacity + 15) // 16 * 16
    values = value_matrix.shape[1]

    flat = token_expert_index.reshape(length * TOP)
    one_hot = flat[:, None] == jnp.arange(n_sp, dtype=jnp.int32)[None, :]
    order = jnp.arange(length * TOP, dtype=jnp.int32)
    earlier = (order[:, None] > order[None, :]).astype(BF16)
    counts = jnp.dot(earlier, one_hot.astype(BF16), preferred_element_type=F32)
    slot = jnp.sum(jnp.where(one_hot, counts, 0.0), axis=1).astype(jnp.int32)
    target = (flat * cap + slot).reshape(length, TOP)

    part = call(
        functools.partial(attention_kernel, n_sp),
        (
            query_matrix,
            key_matrix,
            value_matrix,
            output_gate_rows,
            decay_preactivation,
            channel_decay_bias.reshape(1, width),
            extra_log_decay,
            head_norm_gain.reshape(1, DV),
            output_projection,
        ),
        (0, 1, 2, 3, 4, 8),
        jax.ShapeDtypeStruct((length, model), BF16),
        [
            pltpu.VMEM((DV + FADE_ROWS, width), BF16),
            pltpu.VMEM((n_sp, DV + FADE_ROWS, width), BF16),
            pltpu.VMEM((DV, width), F32),
            pltpu.VMEM((length, values), BF16),
            pltpu.VMEM((length, width), BF16),
            pltpu.VMEM((length, width), BF16),
            pltpu.VMEM((length, values), BF16),
            pltpu.VMEM((length, values), BF16),
            pltpu.VMEM((length, width), BF16),
            pltpu.VMEM((values, model), BF16),
        ]
        + dmas((n_sp,), (n_sp,), (6,)),
        1,
        67043328,
    )
    hidden_units = expert_gate_weight.shape[2]
    by_peer = (n_sp, n_y)
    return call(
        functools.partial(expert_kernel, n_sp, n_tp, cap),
        (
            part,
            residual_input,
            attention_norm_gain.reshape(1, model),
            expert_before_gain.reshape(1, model),
            expert_after_gain.reshape(1, model),
            target,
            target.T,
            routing_weight_matrix,
            expert_gate_weight[0],
            expert_up_weight[0],
            expert_down_weight[0],
        ),
        (1, 8, 9, 10),
        jax.ShapeDtypeStruct((rows, model), BF16),
        [
            pltpu.VMEM((rows, model), BF16),
            pltpu.VMEM((model, hidden_units), BF16),
            pltpu.VMEM((model, hidden_units), BF16),
            pltpu.VMEM((hidden_units, model), BF16),
            pltpu.VMEM((n_y, rows, model), BF16),
            pltpu.VMEM((n_y, rows, model), BF16),
            pltpu.VMEM((n_y, rows, model), BF16),
            pltpu.VMEM((rows, model), BF16),
            pltpu.VMEM((length, share), BF16),
            pltpu.VMEM((n_sp, cap, share), BF16),
            pltpu.VMEM((n_sp, cap, model), BF16),
            pltpu.VMEM((n_sp // 2 * cap, hidden_units), BF16),
            pltpu.VMEM((n_sp, cap, model), BF16),
            pltpu.VMEM(by_peer + (cap, share), BF16),
            pltpu.VMEM(by_peer + (cap, share), BF16),
            pltpu.VMEM(by_peer + (cap, share), BF16),
            pltpu.VMEM((n_sp, cap, share), BF16),
            pltpu.VMEM((n_sp, cap, share), BF16),
            pltpu.VMEM((length, share), BF16),
            pltpu.VMEM((rows, model), BF16),
            pltpu.VMEM((rows, model), BF16),
        ]
        + dmas(
            (4,), (n_y,), (n_y,), (n_y,), (n_y,), (n_tp,), (n_tp,), (n_sp,), (n_sp,),
            (n_y, n_sp), (n_y, n_sp), (n_y, n_sp), (n_y, n_sp),
            by_peer, by_peer, by_peer, by_peer, (n_sp,), (n_sp,), (n_tp,), (n_tp,),
        ),
        2,
        67043328,
    )


def solution(mesh):
    placed = (
        P("sp", "tp"),
        P("sp", "tp"),
        P("sp", "tp"),
        P("sp", "tp"),
        P("sp", "tp"),
        P("tp"),
        P("sp", "tp"),
        P(),
        P("tp", None),
        P(("sp", "tp"), None),
        P(),
        P(),
        P(),
        P("sp", None, "tp"),
        P("sp", None, "tp"),
        P("sp", "tp", None),
        P("sp", None),
        P("sp", None),
    )
    return jax.shard_map(
        functools.partial(shards, mesh.shape["sp"], mesh.shape["tp"]),
        mesh=mesh,
        in_specs=placed,
        out_specs=P(("sp", "tp"), None),
        check_vma=False,
    )
```
